32 devices in a mesh: rep: 2 (over x), fs: 8 (over z, y), tp: 2 (over core).
Axes of the slice: x: 2, y: 2, z: 4, core: 2. Of those that a mesh axis runs over, the one named last changes fastest.
Arguments:
- tokens: bfloat16 [4096, 2048], P(('rep', 'fs', 'tp')), may hold values from -6 to 6
- mix_gain: float32 [2048], replicated, may hold values from 0.1 to 1.9
- conv_in_weight: bfloat16 [2048, 1024], P('fs', 'tp'), may hold values from -0.125 to 0.125
- gate_outer_weight: bfloat16 [2048, 1024], P('fs', 'tp'), may hold values from -0.125 to 0.125
- gate_inner_weight: bfloat16 [2048, 1024], P('fs', 'tp'), may hold values from -0.125 to 0.125
- conv_taps: float32 [3, 1024], P(None, 'tp'), may hold values from -3.5 to 3.5
- out_weight: bfloat16 [1024, 2048], P('tp', 'fs'), may hold values from -0.1875 to 0.1875
- ff_gain: float32 [2048], replicated, may hold values from 0.1 to 1.9
- up_weight: bfloat16 [2048, 8192], P('fs', 'tp'), may hold values from -0.125 to 0.125
- down_weight: bfloat16 [8192, 2048], P('tp', 'fs'), may hold values from -0.0625 to 0.0625
Outputs:
- layer_out: bfloat16 [4096, 2048], P(('rep', 'fs', 'tp'))
The draws below stay inside these ranges and needn't reach their ends.
All inputs are finite; a program needn't handle non-finite values.
Results may differ from the reference program's by a relative error of at most 0.023.
Values may be sent and summed in bfloat16 or wider, within the bound.
No kernel may reach another device: no remote copies, remote signals or barrier semaphores. Data moves between devices by JAX's collectives and lax.ppermute only.
A program may use at most 128 MiB of HBM per device.

```python
import jax
import jax.numpy as jnp
from jax import lax

D = 2048
CONV = 1024
FF = 8192
TAPS = 3
SEQ = 256
TOKENS = 4096
CONV_DEV = 512
FF_DEV = 4096


def block_levels(own_key, extent, shards, least, largest):
    def one(dim, shards_of):
        draws = jax.random.uniform(jax.random.fold_in(jax.random.fold_in(own_key, 6), dim), (shards_of,), jnp.float32, least / len(shards), largest / len(shards))
        return jnp.repeat(jnp.exp(draws), extent[dim] // shards_of).reshape((-1,) + (1,) * (len(extent) - dim - 1))

    loudness = one(*shards[0])
    for cut in shards[1:]:
        loudness = loudness * one(*cut)
    return loudness


def noise(rng, extent, spread, bound, split=(), held_as=jnp.bfloat16):
    result = spread * jax.random.normal(rng, extent, jnp.float32)
    if split:
        result = result * block_levels(rng, extent, split, -0.22, 0.18)
    return jnp.clip(result, -bound, bound).astype(held_as)


def setup_inputs(seed: int = 0) -> dict:
    keys = jax.random.split(jax.random.key(seed), 11)
    tokens = noise(keys[0], (TOKENS, D), 1.0, 6.0, ((0, 32),))
    mix_gain = jnp.clip(1.0 + 0.18 * jax.random.normal(keys[1], (D,), jnp.float32), 0.1, 1.9)
    conv_in_weight = noise(keys[2], (D, CONV), D ** -0.5, 0.125, ((0, 8), (1, 2)))
    gate_outer_weight = noise(keys[3], (D, CONV), D ** -0.5, 0.125, ((0, 8), (1, 2)))
    gate_inner_weight = noise(keys[4], (D, CONV), D ** -0.5, 0.125, ((0, 8), (1, 2)))
    conv_taps = noise(keys[5], (TAPS, CONV), TAPS ** -0.5, 3.5, ((1, 2),), jnp.float32)
    out_weight = noise(keys[6], (CONV, D), CONV ** -0.5, 0.1875, ((0, 2), (1, 8)))
    ff_gain = jnp.clip(1.0 + 0.18 * jax.random.normal(keys[7], (D,), jnp.float32), 0.1, 1.9)
    up_weight = noise(keys[8], (D, FF), D ** -0.5, 0.125, ((0, 8), (1, 2)))
    down_weight = noise(keys[9], (FF, D), FF ** -0.5, 0.0625, ((0, 2), (1, 8)))
    return {"tokens": tokens, "mix_gain": mix_gain, "conv_in_weight": conv_in_weight, "gate_outer_weight": gate_outer_weight, "gate_inner_weight": gate_inner_weight, "conv_taps": conv_taps, "out_weight": out_weight, "ff_gain": ff_gain, "up_weight": up_weight, "down_weight": down_weight}


eps = 1e-06

def rms_scale(values, gain):
    widened = values.astype(jnp.float32)
    inverse = lax.rsqrt(lax.optimization_barrier(jnp.mean(widened * widened, axis=-1, keepdims=True)) + eps)
    return (widened * inverse * gain).astype(jnp.bfloat16)

def block_sum(activ, weight, width):
    blocks = activ.shape[1] // width

    def step(index, total):
        lefts = lax.dynamic_slice_in_dim(activ, index * width, width, 1)
        rights = lax.dynamic_slice_in_dim(weight, index * width, width, 0)
        rounded = jnp.dot(lefts, rights, preferred_element_type=jnp.float32).astype(jnp.bfloat16)
        rounded = lax.optimization_barrier(rounded)
        return total + rounded.astype(jnp.float32)
    initial = jnp.zeros((activ.shape[0], weight.shape[1]), jnp.float32)
    return lax.fori_loop(0, blocks, step, initial)

def reference(tokens, mix_gain, conv_in_weight, gate_outer_weight, gate_inner_weight, conv_taps, out_weight, ff_gain, up_weight, down_weight):
    normed = rms_scale(tokens, mix_gain)
    conv_input = jnp.dot(normed, conv_in_weight, preferred_element_type=jnp.float32).astype(jnp.bfloat16)
    gate_outer = jnp.dot(normed, gate_outer_weight, preferred_element_type=jnp.float32).astype(jnp.bfloat16)
    gate_inner = jnp.dot(normed, gate_inner_weight, preferred_element_type=jnp.float32).astype(jnp.bfloat16)
    gated = gate_inner.astype(jnp.float32) * conv_input.astype(jnp.float32)
    gated = gated.reshape(TOKENS // SEQ, SEQ, CONV)
    padded = jnp.pad(gated, ((0, 0), (TAPS - 1, 0), (0, 0)))
    convolved = conv_taps[0] * padded[:, 0:SEQ] + conv_taps[1] * padded[:, 1:SEQ + 1] + conv_taps[2] * padded[:, 2:SEQ + 2]
    convolved = convolved.reshape(TOKENS, CONV)
    mixed = (gate_outer.astype(jnp.float32) * convolved).astype(jnp.bfloat16)
    resid = (tokens.astype(jnp.float32) + block_sum(mixed, out_weight, CONV_DEV)).astype(jnp.bfloat16)
    normed_ff = rms_scale(resid, ff_gain)
    preact = jnp.dot(normed_ff, up_weight, preferred_element_type=jnp.float32)
    hidden = jnp.square(jax.nn.relu(preact)).astype(jnp.bfloat16)
    return (resid.astype(jnp.float32) + block_sum(hidden, down_weight, FF_DEV)).astype(jnp.bfloat16)
```

```python
import jax
import jax.numpy as jnp
from jax import lax
from jax.sharding import PartitionSpec as P

eps = 1e-06


def rms_scale(values, gain):
    widened = values.astype(jnp.float32)
    inverse = lax.rsqrt(jnp.mean(widened * widened, axis=-1, keepdims=True) + eps)
    return (widened * inverse * gain).astype(jnp.bfloat16)


def after(value, *others):
    return lax.optimization_barrier((value,) + others)[0]


class Layout:
    def __init__(self):
        self.reps, fs, self.cores = (lax.axis_size(a) for a in ("rep", "fs", "tp"))
        self.ys = 2 if fs % 2 == 0 else 1
        self.zs = fs // self.ys
        self.pair = 2 if self.zs % 2 == 0 else 1
        self.parts = self.reps * self.pair
        self.rep, spot, self.core = (lax.axis_index(a) for a in ("rep", "fs", "tp"))
        self.y, self.z = spot % self.ys, spot // self.ys
        self.side = self.z % self.pair

    def _fs(self, move):
        return [(z * self.ys + y, move(z, y)) for z in range(self.zs) for y in range(self.ys)]

    def along_z(self, value, s):
        return lax.ppermute(value, "fs", self._fs(lambda z, y: (z + s) % self.zs * self.ys + y))

    def along_y(self, value, s):
        return lax.ppermute(value, "fs", self._fs(lambda z, y: z * self.ys + (y + s) % self.ys))

    def along_pair(self, value, s):
        n = self.pair
        return lax.ppermute(value, "fs", self._fs(lambda z, y: (z // n * n + (z + s) % n) * self.ys + y))

    def along_rep(self, value, s):
        return lax.ppermute(value, "rep", [(i, (i + s) % self.reps) for i in range(self.reps)])

    def along_tp(self, value, s):
        return lax.ppermute(value, "tp", [(i, (i + s) % self.cores) for i in range(self.cores)])

    def part_for(self, shard, dim, d):
        width = shard.shape[dim] // self.parts
        part = self.rep * self.pair + (self.side + d) % self.pair
        return lax.dynamic_slice_in_dim(shard, part * width, width, dim)

    def spread_z(self, parts):
        return [parts[0]] + [self.along_z(parts[s % self.pair], s) for s in range(1, self.zs)]

    def spread_y(self, came):
        blocks = [((s, 0), block) for s, block in enumerate(came)]
        for t in range(1, self.ys):
            blocks += [((s, t), self.along_y(block, t)) for s, block in enumerate(came)]
        return blocks

    def joined(self, blocks, dim):
        width = blocks[0][1].shape[dim]
        shape = list(blocks[0][1].shape)
        shape[dim] = width * self.zs * self.ys
        whole = jnp.zeros(shape, blocks[0][1].dtype)
        for (s, t), block in blocks:
            at = (self.z - s) % self.zs * self.ys + (self.y - t) % self.ys
            whole = lax.dynamic_update_slice_in_dim(whole, block, at * width, dim)
        return whole

    def members(self):
        return [(a, b) for b in range(self.pair) for a in range(self.reps)]

    def gather_tokens(self, own):
        rows = own.shape[0]
        pieces = {}
        for b in range(self.pair):
            pieces[0, b] = self.along_pair(own, b) if b else own
        for b in range(self.pair):
            for a in range(1, self.reps):
                pieces[a, b] = self.along_rep(pieces[0, b], a)
        sequences = []
        for member in self.members():
            piece = pieces[member]
            sequence = jnp.zeros((self.cores * rows,) + piece.shape[1:], piece.dtype)
            for k in range(self.cores):
                here = self.along_tp(piece, k) if k else piece
                sequence = lax.dynamic_update_slice_in_dim(sequence, here, (self.core - k) % self.cores * rows, 0)
            sequences.append(sequence)
        return jnp.concatenate(sequences, axis=0)

    def scatter_sums(self, partial):
        length = partial.shape[0] // self.parts
        rows = length // self.cores
        sums = {}
        for i, member in enumerate(self.members()):
            sequence = partial[i * length : (i + 1) * length]
            total = None
            for k in range(self.cores):
                block = lax.dynamic_slice_in_dim(sequence, (self.core + k) % self.cores * rows, rows, 0)
                block = (self.along_tp(block, k) if k else block).astype(jnp.float32)
                total = block if total is None else total + block
            sums[member] = total
        lines = []
        for b in range(self.pair):
            line = sums[0, b]
            for a in range(1, self.reps):
                line = line + self.along_rep(sums[a, b].astype(jnp.bfloat16), -a).astype(jnp.float32)
            lines.append(line)
        total = lines[0]
        for b in range(1, self.pair):
            total = total + self.along_pair(lines[b].astype(jnp.bfloat16), -b).astype(jnp.float32)
        return total


def on_device(
    tokens,
    mix_gain,
    conv_in_weight,
    gate_outer_weight,
    gate_inner_weight,
    conv_taps,
    out_weight,
    ff_gain,
    up_weight,
    down_weight,
):
    at = Layout()
    normed = rms_scale(tokens, mix_gain)
    mixer = []
    for d in range(at.pair):
        ins = [at.part_for(w, 1, d) for w in (conv_in_weight, gate_outer_weight, gate_inner_weight)]
        mixer.append(jnp.concatenate(ins + [at.part_for(out_weight, 0, d).T], axis=1))
    mixer_came = at.spread_z(mixer)
    mixer_full = at.joined(at.spread_y(mixer_came), 0)

    up_parts = [after(at.part_for(up_weight, 1, d), *mixer_came[1:]) for d in range(at.pair)]
    up_came = at.spread_z(up_parts)
    up_full = at.joined(at.spread_y(up_came), 0)
    down_parts = [after(at.part_for(down_weight, 0, d), *up_came[1:]) for d in range(at.pair)]
    down_came = at.spread_z(down_parts)
    down_full = at.joined(at.spread_y(down_came), 1)

    gathered = at.gather_tokens(normed)
    channels = mixer_full.shape[1] // 4
    taps = at.part_for(conv_taps, 1, 0)
    projected = jnp.dot(gathered, mixer_full[:, : 3 * channels], preferred_element_type=jnp.float32)
    projected = projected.astype(jnp.bfloat16).astype(jnp.float32)
    projected = projected.reshape(at.parts, -1, 3 * channels)
    conv_input, gate_outer, gate_inner = jnp.split(projected, 3, axis=2)
    gated = gate_inner * conv_input
    length, count = gated.shape[1], taps.shape[0]
    padded = jnp.pad(gated, ((0, 0), (count - 1, 0), (0, 0)))
    convolved = sum(taps[k] * padded[:, k : k + length] for k in range(count))
    mixed = (gate_outer * convolved).astype(jnp.bfloat16).reshape(-1, channels)
    mix_part = lax.dot_general(
        mixed,
        mixer_full[:, 3 * channels :],
        (((1,), (1,)), ((), ())),
        preferred_element_type=jnp.float32,
    ).astype(jnp.bfloat16)
    resid = (tokens.astype(jnp.float32) + at.scatter_sums(mix_part)).astype(jnp.bfloat16)

    ff_gathered = at.gather_tokens(rms_scale(resid, ff_gain))
    preact = jnp.dot(ff_gathered, up_full, preferred_element_type=jnp.float32)
    hidden = jnp.square(jax.nn.relu(preact)).astype(jnp.bfloat16)
    ff_part = jnp.dot(hidden, down_full, preferred_element_type=jnp.float32).astype(jnp.bfloat16)
    return (resid.astype(jnp.float32) + at.scatter_sums(ff_part)).astype(jnp.bfloat16)


def solution(mesh):
    in_specs = (
        P(("rep", "fs", "tp"), None),
        P(),
        P("fs", "tp"),
        P("fs", "tp"),
        P("fs", "tp"),
        P(None, "tp"),
        P("tp", "fs"),
        P(),
        P("fs", "tp"),
        P("tp", "fs"),
    )
    out_specs = P(("rep", "fs", "tp"), None)
    return jax.shard_map(
        on_device, mesh=mesh, in_specs=in_specs, out_specs=out_specs, check_vma=False
    )
```
